32 devices in a mesh: sp: 8 (over z, core), tp: 4 (over y, x).
Axes of the slice: x: 2, y: 2, z: 4, core: 2. Of those that a mesh axis runs over, the one named last changes fastest.
Arguments:
- residual: bfloat16 [1024, 2048], P('sp', 'tp'), may hold values from -48 to 48
- glu_value: bfloat16 [1024, 2048], P('sp', 'tp'), may hold values from -48 to 48
- glu_gate: bfloat16 [1024, 2048], P('sp', 'tp'), may hold values from -6 to 6
- conv_weight: bfloat16 [31, 2048], P(None, 'tp'), may hold values from -1 to 1
- conv_bias: float32 [2048], P('tp'), may hold values from -3 to 3
- ln_gain: float32 [2048], P('tp'), may hold values from 0.1 to 1.9
- ln_bias: float32 [2048], P('tp'), may hold values from -3 to 3
- out_weight: bfloat16 [2048, 2048], P(None, 'tp'), may hold values from -0.125 to 0.125
- norm_gain: float32 [2048], P('tp'), may hold values from 0.1 to 1.9
- route_ids: int32 [1024, 2], P('sp'), may hold values from 0 to 7, all different within a row; in each aligned block of 128 rows (0 to 127, 128 to 255, ...) at most 64 rows name the same one
- route_weight: float32 [1024, 2], P('sp'), may hold values from 0.1 to 1
- expert_gate: bfloat16 [8, 2048, 4096], P('sp', None, 'tp'), may hold values from -0.125 to 0.125
- expert_up: bfloat16 [8, 2048, 4096], P('sp', None, 'tp'), may hold values from -0.125 to 0.125
- expert_down: bfloat16 [8, 4096, 2048], P('sp', 'tp'), may hold values from -0.09375 to 0.09375
Outputs:
- layer_out: bfloat16 [1024, 2048], P('sp', 'tp')
The draws below stay inside these ranges and needn't reach their ends.
Inputs may be any that keep to these rules, and one draw needn't show every extreme that they name: `route_ids`: within the 128 rows of one index of sp, no expert is named more than 64 times, and in some such rows one expert is named exactly 64 times.
All inputs are finite; a program needn't handle non-finite values.
Results may differ from the reference program's by a relative error of at most 0.006.
Values may be sent and summed in bfloat16 or wider, within the bound.
No kernel may reach another device: no remote copies, remote signals or barrier semaphores. Data moves between devices by JAX's collectives and lax.ppermute only.
A program may use at most 64 MiB of HBM per device.

```python
import math
import jax
import jax.numpy as jnp
import numpy as np
from jax import lax

D = 2048
FF = 4096
KERNEL = 31
TOPK = 2
ROWS = 128
TOKENS = 1024
EXPERTS = 8
CAP = 64
N_SP = 8
N_TP = 4


def rising_field(key, low, high):
    ramp = jnp.exp(jnp.linspace(math.log(low), math.log(high), D)).astype(jnp.float32)
    base = jnp.clip(jax.random.normal(key, (TOKENS, D), jnp.float32), -6.0, 6.0)
    return base * ramp


def draw_residual(key, part):
    return rising_field(jax.random.fold_in(key, 11), 0.5, 2.0).astype(jnp.bfloat16)


def draw_glu_value(key, part):
    return rising_field(jax.random.fold_in(key, 23), 0.5, 2.0).astype(jnp.bfloat16)


def levels(stream_key, dims, shards, least, largest):
    def one(position, parts):
        heights = jax.random.uniform(jax.random.fold_in(jax.random.fold_in(stream_key, 6), position), (parts,), jnp.float32, least / len(shards), largest / len(shards))
        return jnp.repeat(jnp.exp(heights), dims[position] // parts).reshape((-1,) + (1,) * (len(dims) - position - 1))

    loudness = one(*shards[0])
    for cut in shards[1:]:
        loudness = loudness * one(*cut)
    return loudness


def routed_block(rng, own, number, rows, count, top, most, skew):
    order = jax.random.permutation(rng, count)
    heavy_load, ordinary = portions_of(count, rows * top, most, skew, True), portions_of(count, rows * top, most, skew, False)
    places = jnp.arange(count)

    def named(lengths, turn):
        used = int((lengths > 0).sum())
        fixed = max(1, used // 4)
        moved = fixed + (places - fixed + turn * (used - fixed)) % max(1, count - fixed)
        return jnp.zeros((count,), jnp.int32).at[order[jnp.where(places < fixed, places, moved)]].set(jnp.asarray(lengths, jnp.int32))

    lengths = jnp.where(number % 4 == 0, named(heavy_load, number // 4), named(ordinary, number - number // 4 - 1))
    mixed = jax.random.permutation(jax.random.fold_in(own, 3), count)
    giver, sink = mixed[0:count // 2 * 2:2], mixed[1:count // 2 * 2:2]
    slack = jnp.minimum(lengths[giver] - 1, most - lengths[sink]) // 2
    slack = jnp.where((giver == order[0]) | (sink == order[0]) | (lengths[sink] == 0), 0, jnp.maximum(slack, 0))
    moved = jax.random.randint(jax.random.fold_in(own, 4), (count // 2,), 0, 1 << 20) % (slack + 1)
    lengths = lengths.at[giver].add(-moved).at[sink].add(moved)
    items = jnp.searchsorted(jnp.cumsum(lengths), jnp.arange(rows * top), side="right").astype(jnp.int32)
    table = items.reshape(top, rows).T
    table = table[jax.random.permutation(jax.random.fold_in(own, 1), rows)]
    turn = jax.random.randint(jax.random.fold_in(own, 2), (rows, 1), 0, top)
    return jnp.take_along_axis(table, (jnp.arange(top)[None, :] + turn) % top, axis=1)


def portions_of(count, total, bound, lean, full):
    loads = [(1 << 20) // math.isqrt(rank ** lean) + 1 for rank in range(1, count + 1)]
    largest = bound if full else min(bound, max(-(-total // count), total * loads[0] // sum(loads)))
    least = 1 if total - largest >= count - 1 else 0
    counts, spare = [largest] + [least] * (count - 1), total - largest - least * (count - 1)
    while spare > 0:
        candidates = [i for i in range(1, count) if counts[i] < largest] or [i for i in range(1, count) if counts[i] < bound]
        whole, left = sum([loads[i] for i in candidates]), spare
        for i in candidates:
            extra = min(bound - counts[i], max(1, left * loads[i] // whole), spare)
            counts[i] = counts[i] + extra
            spare = spare - extra
    return np.array(counts)


def gaussian(rng, shape, spread, limit, cuts=(), kind=jnp.bfloat16):
    drawn = spread * jax.random.normal(rng, shape, jnp.float32)
    if cuts:
        drawn = drawn * levels(rng, shape, cuts, -0.22, 0.18)
    return jnp.clip(drawn, -limit, limit).astype(kind)


def setup_inputs(seed: int = 0) -> dict:
    arg_keys = jax.random.split(jax.random.key(seed), 15)
    residual = draw_residual(jax.random.fold_in(arg_keys[14], 71), 0)
    glu_value = draw_glu_value(jax.random.fold_in(arg_keys[14], 71), 0)
    glu_gate = gaussian(arg_keys[2], (TOKENS, D), 1.0, 6.0, ((0, 8), (1, 4)))
    conv_weight = gaussian(arg_keys[3], (KERNEL, D), KERNEL ** -0.5, 1.0, ((1, 4),))
    conv_bias = gaussian(arg_keys[4], (D,), 0.5, 3.0, ((0, 4),), jnp.float32)
    ln_gain = jnp.clip(1.0 + 0.18 * jax.random.normal(arg_keys[5], (D,), jnp.float32), 0.1, 1.9)
    ln_bias = gaussian(arg_keys[6], (D,), 0.5, 3.0, ((0, 4),), jnp.float32)
    out_weight = gaussian(arg_keys[7], (D, D), D ** -0.5, 0.125, ((1, 4),))
    norm_gain = jnp.clip(1.0 + 0.18 * jax.random.normal(arg_keys[8], (D,), jnp.float32), 0.1, 1.9)
    route_ids_keys = jax.random.split(jax.random.fold_in(arg_keys[9], 1), TOKENS // ROWS)
    route_ids_turns = jax.random.permutation(jax.random.fold_in(arg_keys[9], 3), TOKENS // ROWS)
    route_ids = jax.vmap(lambda own, number: routed_block(jax.random.fold_in(arg_keys[9], 2), own, number, ROWS, EXPERTS, TOPK, CAP, 2))(route_ids_keys, route_ids_turns).reshape((TOKENS, TOPK))
    route_weight = jnp.clip(jnp.exp(math.log(1.0) - 2.3025851 * jax.random.uniform(arg_keys[10], (TOKENS, TOPK), jnp.float32) ** levels(arg_keys[10], (TOKENS, TOPK), ((0, 8),), -0.2, 0.2)), 0.1, 1.0)
    expert_gate = gaussian(arg_keys[11], (EXPERTS, D, FF), D ** -0.5, 0.125, ((0, 8), (2, 4)))
    expert_up = gaussian(arg_keys[12], (EXPERTS, D, FF), D ** -0.5, 0.125, ((0, 8), (2, 4)))
    expert_down = gaussian(arg_keys[13], (EXPERTS, FF, D), FF ** -0.5, 0.09375, ((0, 8), (1, 4)))
    return dict(residual=residual, glu_value=glu_value, glu_gate=glu_gate, conv_weight=conv_weight, conv_bias=conv_bias, ln_gain=ln_gain, ln_bias=ln_bias, out_weight=out_weight, norm_gain=norm_gain, route_ids=route_ids, route_weight=route_weight, expert_gate=expert_gate, expert_up=expert_up, expert_down=expert_down)


def reference(residual, glu_value, glu_gate, conv_weight, conv_bias, ln_gain, ln_bias, out_weight, norm_gain, route_ids, route_weight, expert_gate, expert_up, expert_down):
    gated = (glu_value.astype(jnp.float32) * jax.nn.sigmoid(glu_gate.astype(jnp.float32))).astype(jnp.bfloat16)
    reach = KERNEL // 2
    padded = jnp.pad(gated.astype(jnp.float32), ((reach, reach), (0, 0)))
    taps = conv_weight.astype(jnp.float32)
    conv = jnp.zeros(gated.shape, jnp.float32) + conv_bias
    for tap in range(KERNEL):
        conv = conv + padded[tap:tap + TOKENS] * taps[tap]
    mean = lax.optimization_barrier(jnp.mean(conv, axis=1, keepdims=True))
    var = lax.optimization_barrier(jnp.mean(conv * conv, axis=1, keepdims=True)) - mean * mean
    act = jax.nn.silu((conv - mean) * lax.rsqrt(var + 1e-05) * ln_gain + ln_bias).astype(jnp.bfloat16)
    mixed = residual.astype(jnp.float32) + jnp.dot(act, out_weight, preferred_element_type=jnp.float32)
    squares = lax.optimization_barrier(jnp.mean(mixed * mixed, axis=1, keepdims=True))
    normed = (mixed * lax.rsqrt(squares + 1e-06) * norm_gain).astype(jnp.bfloat16)
    flat = route_ids.reshape(-1)
    owner = (jnp.arange(TOKENS * TOPK, dtype=jnp.int32) // TOPK).astype(jnp.int32)
    weights = route_weight.reshape(-1)
    slots = N_SP * CAP
    slot_index = jnp.arange(slots, dtype=jnp.int32)
    block = FF // N_TP

    def per_expert(total, expert):
        chosen = flat == expert
        picks = jnp.nonzero(chosen, size=slots, fill_value=0)[0].astype(jnp.int32)
        count = jnp.sum(chosen.astype(jnp.int32))
        live = (slot_index < count).astype(jnp.float32)
        rows = normed[owner[picks]]
        gate = jnp.dot(rows, expert_gate[expert], preferred_element_type=jnp.float32)
        up = jnp.dot(rows, expert_up[expert], preferred_element_type=jnp.float32)
        hidden = (jax.nn.silu(gate) * up).astype(jnp.bfloat16)
        down = expert_down[expert]
        result = jnp.zeros((slots, D), jnp.float32)
        for part_index in range(N_TP):
            piece = jnp.dot(hidden[:, part_index * block:(part_index + 1) * block], down[part_index * block:(part_index + 1) * block], preferred_element_type=jnp.float32)
            result = result + piece.astype(jnp.bfloat16).astype(jnp.float32)
        result = result.astype(jnp.bfloat16)
        scaled = result.astype(jnp.float32) * (weights[picks] * live)[:, None]
        return (total.at[owner[picks]].add(scaled), None)
    moe, _ = lax.scan(per_expert, jnp.zeros((TOKENS, D), jnp.float32), jnp.arange(EXPERTS, dtype=jnp.int32))
    return (mixed + moe).astype(jnp.bfloat16)
```

```python
import functools

import jax
import jax.numpy as jnp
from jax import lax
from jax.experimental import pallas as pl
from jax.experimental.pallas import tpu as pltpu
from jax.sharding import PartitionSpec as P

F32 = jnp.float32
BF16 = jnp.bfloat16
SUB = 16
LANES = 128
VMEM_SPEC = pl.BlockSpec(memory_space=pltpu.VMEM)
SMEM_SPEC = pl.BlockSpec(memory_space=pltpu.SMEM)


def swap(value, axis, offset):
    count = lax.axis_size(axis)
    return lax.ppermute(value, axis, [(i, i ^ offset) for i in range(count)])


def spread(value, axis):
    return [value] + [swap(value, axis, k) for k in range(1, lax.axis_size(axis))]


def route_kernel(here, ids, slots_col, slots_row, *, capacity):
    rows = ids.shape[0]
    topk = ids.shape[1]
    lane = lax.broadcasted_iota(jnp.int32, (rows, LANES), 1)
    row = lax.broadcasted_iota(jnp.int32, (rows, rows), 0)
    col = lax.broadcasted_iota(jnp.int32, (rows, rows), 1)
    earlier = jnp.where(col < row, 1.0, 0.0).astype(BF16)
    hits = [jnp.where(lane == ids[:, k : k + 1], 1.0, 0.0) for k in range(topk)]
    before = jnp.dot(earlier, sum(hits).astype(BF16), preferred_element_type=F32)
    rowform = []
    colform = jnp.zeros((rows, LANES), jnp.int32)
    for k in range(topk):
        rank = jnp.sum(before * hits[k], axis=1, keepdims=True).astype(jnp.int32)
        slot = (ids[:, k : k + 1] ^ here[0]) * capacity + rank
        colform = jnp.where(lane == k, slot, colform)
        wide = jnp.broadcast_to(slot.astype(F32), (rows, rows))
        rowform.append(wide.T[:8].astype(jnp.int32))
    slots_col[...] = colform
    sub = lax.broadcasted_iota(jnp.int32, (8, rows), 0)
    out = rowform[0]
    for k in range(1, topk):
        out = jnp.where(sub == k, rowform[k], out)
    slots_row[...] = out


def conv_kernel(before, gated, after, taps, bias, gain, shift, scale, out, padded):
    rows, width = gated.shape
    edge = before.shape[0]
    count = taps.shape[0]
    reach = count // 2
    padded[:edge] = before[...].astype(F32)
    padded[edge : edge + rows] = gated[...].astype(F32)
    padded[edge + rows :] = after[...].astype(F32)
    first = edge - reach
    sums = jnp.zeros((rows, LANES), F32)
    pieces = []
    for lo in range(0, width, LANES):
        part = slice(lo, lo + LANES)
        weights = taps[:, part].astype(F32)
        acc = jnp.broadcast_to(bias[:, part], (rows, LANES))
        for turn in range(8):
            mine = [t for t in range(count) if (t + first) % 8 == turn]
            if not mine:
                continue
            top = max((t + first) // 8 for t in mine) * 8
            moved = padded[turn : turn + top + rows, part]
            for t in mine:
                at = (t + first) // 8 * 8
                acc = acc + moved[at : at + rows] * weights[t : t + 1]
        pieces.append(acc)
        sums = sums + acc
    mean = jnp.sum(sums, axis=1, keepdims=True) * (1.0 / width)
    pivot = mean.astype(BF16).astype(F32)
    for i, acc in enumerate(pieces):
        out[:rows, i * LANES : (i + 1) * LANES] = (acc - pivot).astype(BF16)
    line = jnp.broadcast_to(pivot, (rows, rows)).T[:SUB]
    sub = lax.broadcasted_iota(jnp.int32, (SUB, width), 0)
    if width > rows:
        line = jnp.concatenate([line, jnp.zeros((SUB, width - rows), F32)], axis=1)
    tail = line
    at = 1
    for vector in (gain, shift, scale):
        left = vector[...]
        for _ in range(3):
            piece = left.astype(BF16).astype(F32)
            tail = jnp.where(sub == at, piece, tail)
            left = left - piece
            at += 1
    out[rows:] = jnp.where(sub < at, tail, 0.0).astype(BF16)


def mix_kernel(here, *refs, peers, spots, capacity, topk):
    exts = refs[:peers]
    weight, residual, slots_row, mixed_out, inverse = refs[peers : peers + 5]
    outgoing = refs[peers + 5 :]
    rows, width = residual.shape
    total = width * peers
    sums = jnp.zeros((rows, LANES), F32)
    pivots = []
    for k in range(peers):
        line = exts[k][rows : rows + 8, :rows].astype(F32)[:1]
        pivot = jnp.broadcast_to(line, (rows, rows)).T[:, :1]
        pivots.append(pivot)
        part = exts[k][:rows].astype(F32)
        for lo in range(0, width, LANES):
            sums = sums + part[:, lo : lo + LANES]
    mean = jnp.sum(sums, axis=1, keepdims=True) * (1.0 / total)
    mean = mean + sum(pivots) * (1.0 / peers)
    squares = jnp.zeros((rows, LANES), F32)
    for k in range(peers):
        part = exts[k][:rows].astype(F32) + (pivots[k] - mean)
        part = part * part
        for lo in range(0, width, LANES):
            squares = squares + part[:, lo : lo + LANES]
    var = jnp.sum(squares, axis=1, keepdims=True) * (1.0 / total)
    rate = lax.rsqrt(var + 1e-05)
    acc = residual[...].astype(F32)
    rowid = lax.broadcasted_iota(jnp.int32, (inverse.shape[0], width), 0)
    inverses = jnp.zeros((inverse.shape[0], width), F32)
    own_scale = None
    for k in range(peers):
        extra = exts[k][rows:].astype(F32)
        gain = extra[1:2] + extra[2:3] + extra[3:4]
        shift = extra[4:5] + extra[5:6] + extra[6:7]
        scale = extra[7:8] + extra[8:9] + extra[9:10]
        if k == 0:
            own_scale = scale
        inverses = jnp.where(rowid == k, 1.0 / scale, inverses)
        pre = (exts[k][:rows].astype(F32) + (pivots[k] - mean)) * rate * gain + shift
        act = (pre / (1.0 + jnp.exp(-pre))).astype(BF16)
        start = pl.multiple_of((here[1] ^ k) * width, width)
        acc = acc + jnp.dot(act, weight[pl.ds(start, width), :], preferred_element_type=F32)
    inverse[...] = inverses
    mixed_out[...] = acc
    scaled = (acc * own_scale).astype(BF16)
    for d in range(spots):
        slot = lax.broadcasted_iota(jnp.int32, (capacity, rows), 0) + d * capacity
        match = slot == slots_row[0:1]
        for j in range(1, topk):
            match = match | (slot == slots_row[j : j + 1])
        chosen = jnp.where(match, 1.0, 0.0).astype(BF16)
        outgoing[d][...] = jnp.dot(chosen, scaled, preferred_element_type=F32).astype(BF16)


def ffn_kernel(here, *refs, peers):
    blocks = refs[:peers]
    inverse, gate_w, up_w, down_w = refs[peers : peers + 4]
    outs = refs[peers + 4 : 2 * peers + 4]
    gate_acc, up_acc, square_acc, hidden = refs[2 * peers + 4 :]
    step = pl.program_id(0)
    width = blocks[0].shape[1]
    for k in range(peers):

        @pl.when(step == k)
        def _(k=k):
            x = blocks[k][...]
            gate = jnp.dot(x, gate_w[...], preferred_element_type=F32)
            up = jnp.dot(x, up_w[...], preferred_element_type=F32)
            plain = x.astype(F32) * inverse[k : k + 1]
            plain = plain * plain
            folded = plain[:, :LANES]
            for lo in range(LANES, width, LANES):
                folded = folded + plain[:, lo : lo + LANES]
            if k == 0:
                gate_acc[...] = gate
                up_acc[...] = up
                square_acc[...] = folded
            else:
                gate_acc[...] += gate
                up_acc[...] += up
                square_acc[...] += folded

    @pl.when(step == peers)
    def _():
        squares = jnp.sum(square_acc[...], axis=1, keepdims=True)
        rate = lax.rsqrt(squares * (1.0 / (width * peers)) + 1e-06)
        gate = gate_acc[...] * rate
        up = up_acc[...] * rate
        hidden[...] = (gate / (1.0 + jnp.exp(-gate)) * up).astype(BF16)

    for k in range(peers):

        @pl.when(step == peers + k)
        def _(k=k):
            outs[k][...] = jnp.dot(hidden[...], down_w[...], preferred_element_type=F32).astype(
                BF16
            )


def combine_kernel(*refs, spots, topk):
    pieces = refs[:spots]
    slots_col, weights, mixed, out = refs[spots:]
    rows = mixed.shape[0]
    capacity = pieces[0].shape[0]
    table = jnp.concatenate([piece[...] for piece in pieces], axis=0)
    slot = lax.broadcasted_iota(jnp.int32, (rows, spots * capacity), 1)
    total = mixed[...]
    for k in range(topk):
        chosen = jnp.where(slot == slots_col[:, k : k + 1], 1.0, 0.0).astype(BF16)
        picked = jnp.dot(chosen, table, preferred_element_type=F32)
        total = total + picked * weights[:, k : k + 1]
    out[...] = total.astype(BF16)


def on_device(
    residual,
    glu_value,
    glu_gate,
    conv_weight,
    conv_bias,
    ln_gain,
    ln_bias,
    out_weight,
    norm_gain,
    route_ids,
    route_weight,
    expert_gate,
    expert_up,
    expert_down,
):
    rows, width = residual.shape
    spots = lax.axis_size("sp")
    peers = lax.axis_size("tp")
    topk = route_ids.shape[1]
    capacity = 2 * rows * topk // spots
    hidden_units = expert_gate.shape[2]
    here = jnp.stack([lax.axis_index("sp"), lax.axis_index("tp")]).astype(jnp.int32)

    gated = (glu_value.astype(F32) * jax.nn.sigmoid(glu_gate.astype(F32))).astype(BF16)
    reach = conv_weight.shape[0] // 2
    edge = -(-reach // SUB) * SUB
    ends = spots - 1
    before = lax.ppermute(gated[rows - edge :], "sp", [(i, i + 1) for i in range(ends)])
    after = lax.ppermute(gated[:edge], "sp", [(i + 1, i) for i in range(ends)])

    slots_col, slots_row = pl.pallas_call(
        functools.partial(route_kernel, capacity=capacity),
        out_shape=(
            jax.ShapeDtypeStruct((rows, LANES), jnp.int32),
            jax.ShapeDtypeStruct((8, rows), jnp.int32),
        ),
        in_specs=[SMEM_SPEC, VMEM_SPEC],
        out_specs=(VMEM_SPEC, VMEM_SPEC),
        name="route",
    )(here, route_ids)

    ext = pl.pallas_call(
        conv_kernel,
        out_shape=jax.ShapeDtypeStruct((rows + SUB, width), BF16),
        in_specs=[VMEM_SPEC] * 8,
        out_specs=VMEM_SPEC,
        scratch_shapes=[pltpu.VMEM((rows + 2 * edge, width), F32)],
        name="conv",
    )(
        before,
        gated,
        after,
        conv_weight,
        conv_bias[None],
        ln_gain[None],
        ln_bias[None],
        norm_gain[None],
    )
    exts = spread(ext, "tp")

    padded_peers = -(-peers // 8) * 8
    mixed, inverse, *outgoing = pl.pallas_call(
        functools.partial(
            mix_kernel, peers=peers, spots=spots, capacity=capacity, topk=topk
        ),
        out_shape=[
            jax.ShapeDtypeStruct((rows, width), F32),
            jax.ShapeDtypeStruct((padded_peers, width), F32),
        ]
        + [jax.ShapeDtypeStruct((capacity, width), BF16)] * spots,
        in_specs=[SMEM_SPEC] + [VMEM_SPEC] * (peers + 3),
        out_specs=[VMEM_SPEC] * (spots + 2),
        name="mix",
    )(here, *exts, out_weight, residual, slots_row)

    arrived = [outgoing[0]] + [swap(outgoing[d], "sp", d) for d in range(1, spots)]

    def expert(chunk):
        blocks = spread(chunk, "tp")
        size = chunk.shape[0]
        full = lambda *_: (0, 0)
        k_of = lambda i: jnp.minimum(i, peers - 1)
        n_of = lambda i: jnp.maximum(i - peers, 0)
        spec = pltpu.PrefetchScalarGridSpec(
            num_scalar_prefetch=1,
            grid=(2 * peers,),
            in_specs=[pl.BlockSpec((size, width), full)] * peers
            + [
                pl.BlockSpec((padded_peers, width), full),
                pl.BlockSpec((None, width, hidden_units), lambda i, h: (0, h[1] ^ k_of(i), 0)),
                pl.BlockSpec((None, width, hidden_units), lambda i, h: (0, h[1] ^ k_of(i), 0)),
                pl.BlockSpec((None, hidden_units, width), lambda i, h: (0, 0, h[1] ^ n_of(i))),
            ],
            out_specs=[pl.BlockSpec((size, width), full)] * peers,
            scratch_shapes=[
                pltpu.VMEM((size, hidden_units), F32),
                pltpu.VMEM((size, hidden_units), F32),
                pltpu.VMEM((size, LANES), F32),
                pltpu.VMEM((size, hidden_units), BF16),
            ],
        )
        parts = pl.pallas_call(
            functools.partial(ffn_kernel, peers=peers),
            grid_spec=spec,
            out_shape=[jax.ShapeDtypeStruct((size, width), BF16)] * peers,
            name="ffn",
        )(here, *blocks, inverse, expert_gate, expert_up, expert_down)
        total = parts[0].astype(F32)
        for k in range(1, peers):
            total = total + swap(parts[k], "tp", k).astype(F32)
        return total.astype(BF16)

    half = spots // 2
    near = expert(jnp.concatenate(arrived[:half], axis=0))
    far = expert(jnp.concatenate(arrived[half:], axis=0))
    back = []
    for d in range(spots):
        source, at = (near, d) if d < half else (far, d - half)
        piece = source[at * capacity : (at + 1) * capacity]
        back.append(piece if d == 0 else swap(piece, "sp", d))

    return pl.pallas_call(
        functools.partial(combine_kernel, spots=spots, topk=topk),
        out_shape=jax.ShapeDtypeStruct((rows, width), BF16),
        in_specs=[VMEM_SPEC] * (spots + 3),
        out_specs=VMEM_SPEC,
        name="combine",
    )(*back, slots_col, route_weight, mixed)


def solution(mesh):
    in_specs = (
        P("sp", "tp"),
        P("sp", "tp"),
        P("sp", "tp"),
        P(None, "tp"),
        P("tp"),
        P("tp"),
        P("tp"),
        P(None, "tp"),
        P("tp"),
        P("sp", None),
        P("sp", None),
        P("sp", None, "tp"),
        P("sp", None, "tp"),
        P("sp", "tp", None),
    )
    out_specs = P("sp", "tp")
    return jax.shard_map(
        on_device, mesh=mesh, in_specs=in_specs, out_specs=out_specs, check_vma=False
    )
```
